32 devices in a mesh: rep: 2 (over y), fs: 4 (over z), tp: 4 (over x, core).
Axes of the slice: x: 2, y: 2, z: 4, core: 2. Of those that a mesh axis runs over, the one named last changes fastest.
Arguments:
- activations: bfloat16 [3072, 2048], P(('rep', 'fs'), 'tp'), may hold values from -16 to 16
- norm_gain: float32 [2048], replicated, may hold values from 0.1 to 1.9
- query_weight: bfloat16 [2048, 512], P('fs', 'tp'), may hold values from -0.125 to 0.125
- key_weight: bfloat16 [2048, 512], P('fs', 'tp'), may hold values from -0.125 to 0.125
- value_weight: bfloat16 [2048, 512], P('fs', 'tp'), may hold values from -0.125 to 0.125
- gate_weight: bfloat16 [2048, 512], P('fs', 'tp'), may hold values from -0.125 to 0.125
- out_weight: bfloat16 [512, 2048], P('tp', 'fs'), may hold values from -0.25 to 0.25
- mlp_gain: float32 [2048], replicated, may hold values from 0.1 to 1.9
- up_weight: bfloat16 [2048, 8192], P('fs', 'tp'), may hold values from -0.125 to 0.125
- down_weight: bfloat16 [8192, 2048], P('tp', 'fs'), may hold values from -0.0625 to 0.0625
Outputs:
- layer_out: bfloat16 [3072, 2048], P(('rep', 'fs'), 'tp')
The draws below stay inside these ranges and needn't reach their ends.
All inputs are finite; a program needn't handle non-finite values.
Results may differ from the reference program's by a relative error of at most 0.012.
Values may be sent and summed in bfloat16 or wider, within the bound.
A program may use at most 64 MiB of HBM per device.

```python
import math
import jax
import jax.numpy as jnp
from jax import lax

D = 2048
FF = 8192
HEADS = 8
HEAD_DIM = 64
BLOCK = 64
SEQ_LEN = 128
TOKENS = 3072
N_TP = 4


def draw_activations(key, part):
    key_base, key_column, key_row = jax.random.split(jax.random.fold_in(key, 11), 3)
    column_index = jnp.arange(D, dtype=jnp.float32)
    column_scale = jnp.power(3.0, column_index / (D - 1)) * jnp.exp(jax.random.uniform(key_column, (D,), jnp.float32, -0.35, 0.35))
    base_draw = jax.random.normal(key_base, (TOKENS, D), jnp.float32)
    row_scale = jnp.exp(jax.random.uniform(key_row, (TOKENS, 1), jnp.float32, 0.0, math.log(4.0)))
    return jnp.clip(0.5 * base_draw * row_scale * column_scale[None, :], -16.0, 16.0).astype(jnp.bfloat16)


def level_of(key, shape, cuts, least, largest):
    loudness = 1.0
    for dim, shards_of in cuts:
        steps = jax.random.uniform(jax.random.fold_in(jax.random.fold_in(key, 6), dim), (shards_of,), jnp.float32, least / len(cuts), largest / len(cuts))
        loudness = loudness * jnp.repeat(jnp.exp(steps), shape[dim] // shards_of).reshape((-1,) + (1,) * (len(shape) - 1 - dim))
    return loudness


def noise(key, extent, scale, bound, cuts=(), kind=jnp.bfloat16):
    factor_of = level_of(key, extent, cuts, -0.22, 0.18) if cuts else 1.0
    values = jax.random.normal(key, extent, jnp.float32) * scale * factor_of
    return jnp.minimum(jnp.maximum(values, -bound), bound).astype(kind)


def setup_inputs(seed: int = 0) -> dict:
    streams_of = jax.random.split(jax.random.key(seed), 11)
    return {
        "activations": draw_activations(jax.random.fold_in(streams_of[10], 71), 0),
        "norm_gain": jnp.clip(1.0 + 0.18 * jax.random.normal(streams_of[1], (D,), jnp.float32), 0.1, 1.9),
        "query_weight": noise(streams_of[2], (D, HEADS * HEAD_DIM), D ** -0.5, 0.125, ((0, 4), (1, 4))),
        "key_weight": noise(streams_of[3], (D, HEADS * HEAD_DIM), D ** -0.5, 0.125, ((0, 4), (1, 4))),
        "value_weight": noise(streams_of[4], (D, HEADS * HEAD_DIM), D ** -0.5, 0.125, ((0, 4), (1, 4))),
        "gate_weight": noise(streams_of[5], (D, HEADS * HEAD_DIM), D ** -0.5, 0.125, ((0, 4), (1, 4))),
        "out_weight": noise(streams_of[6], (HEADS * HEAD_DIM, D), (HEADS * HEAD_DIM) ** -0.5, 0.25, ((0, 4), (1, 4))),
        "mlp_gain": jnp.clip(1.0 + 0.18 * jax.random.normal(streams_of[7], (D,), jnp.float32), 0.1, 1.9),
        "up_weight": noise(streams_of[8], (D, FF), D ** -0.5, 0.125, ((0, 4), (1, 4))),
        "down_weight": noise(streams_of[9], (FF, D), FF ** -0.5, 0.0625, ((0, 4), (1, 4))),
    }


EPSILON = 1e-06

def rms_norm(rows, gain):
    floats = rows.astype(jnp.float32)
    scaled = floats * lax.rsqrt(lax.optimization_barrier(jnp.mean(floats * floats, axis=-1, keepdims=True)) + EPSILON)
    return (scaled * gain.astype(jnp.float32)).astype(jnp.bfloat16)

def rotate(raw, cosine, sine, seqs, heads):
    half = HEAD_DIM // 2
    shaped = raw.reshape(seqs, SEQ_LEN, heads, HEAD_DIM)
    first, second = (shaped[..., :half], shaped[..., half:])
    return jnp.concatenate([first * cosine - second * sine, second * cosine + first * sine], axis=-1)

def retain(query_raw, key_raw, value_rows, gate_rows, first_head):
    tokens = query_raw.shape[0]
    heads = query_raw.shape[1] // HEAD_DIM
    seqs = tokens // SEQ_LEN
    blocks = SEQ_LEN // BLOCK
    half = HEAD_DIM // 2
    position = jnp.arange(SEQ_LEN, dtype=jnp.float32)
    freqs = 10000.0 ** (-jnp.arange(half, dtype=jnp.float32) / half)
    angle = position[:, None] * freqs[None, :]
    cosine = jnp.cos(angle)[:, None, :]
    sine = jnp.sin(angle)[:, None, :]
    shape_five = (seqs, blocks, BLOCK, heads, HEAD_DIM)
    queries = rotate(query_raw, cosine, sine, seqs, heads).astype(jnp.bfloat16).reshape(shape_five)
    key_block = (rotate(key_raw, cosine, sine, seqs, heads) * HEAD_DIM ** (-0.5)).astype(jnp.bfloat16).reshape(shape_five)
    value_block = value_rows.reshape(shape_five)
    head_index = first_head + jnp.arange(heads, dtype=jnp.float32)
    exponent = 5.0 + 4.0 * head_index / (HEADS - 1)
    log_gamma = jnp.log(1.0 - jnp.power(2.0, -exponent))
    offsets = jnp.arange(BLOCK, dtype=jnp.float32)
    distance = offsets[:, None] - offsets[None, :]
    decay_mask = jnp.where(distance[None] >= 0, jnp.exp(jnp.maximum(distance, 0.0)[None] * log_gamma[:, None, None]), 0.0)
    scores = jnp.einsum('snbhd,snchd->snhbc', queries.astype(jnp.float32), key_block.astype(jnp.float32))
    weights = (scores * decay_mask[None, None]).astype(jnp.bfloat16)
    inner = jnp.einsum('snhbc,snchd->snbhd', weights.astype(jnp.float32), value_block.astype(jnp.float32))
    query_decay = queries.astype(jnp.float32) * jnp.exp((offsets + 1.0)[:, None] * log_gamma[None, :])[:, :, None]
    key_decay = key_block.astype(jnp.float32) * jnp.exp((BLOCK - 1.0 - offsets)[:, None] * log_gamma[None, :])[:, :, None]
    block_decay = jnp.exp(BLOCK * log_gamma)[None, :, None, None]

    def advance(state, inputs):
        query_now, key_now, value_now = inputs
        carried = jnp.einsum('sbhd,shde->sbhe', query_now, state, precision=lax.Precision.HIGHEST)
        state = state * block_decay + jnp.einsum('sbhd,sbhe->shde', key_now, value_now, precision=lax.Precision.HIGHEST)
        return (state, carried)
    initial = jnp.zeros((seqs, heads, HEAD_DIM, HEAD_DIM), jnp.float32)
    _, cross = lax.scan(advance, initial, (jnp.moveaxis(query_decay, 1, 0), jnp.moveaxis(key_decay, 1, 0), jnp.moveaxis(value_block.astype(jnp.float32), 1, 0)))
    mixed = (inner + jnp.moveaxis(cross, 0, 1)).reshape(tokens, heads, HEAD_DIM)
    centred = mixed - lax.optimization_barrier(jnp.mean(mixed, axis=-1, keepdims=True))
    normed = centred * lax.rsqrt(lax.optimization_barrier(jnp.mean(centred * centred, axis=-1, keepdims=True)) + EPSILON)
    gated = normed * jax.nn.silu(gate_rows.reshape(tokens, heads, HEAD_DIM))
    return gated.reshape(tokens, heads * HEAD_DIM).astype(jnp.bfloat16)

def reference(activations, norm_gain, query_weight, key_weight, value_weight, gate_weight, out_weight, mlp_gain, up_weight, down_weight):
    normed = rms_norm(activations, norm_gain)
    query_raw = jnp.dot(normed, query_weight, preferred_element_type=jnp.float32)
    key_raw = jnp.dot(normed, key_weight, preferred_element_type=jnp.float32)
    value_rows = jnp.dot(normed, value_weight, preferred_element_type=jnp.float32).astype(jnp.bfloat16)
    gate_rows = jnp.dot(normed, gate_weight, preferred_element_type=jnp.float32)
    retained = retain(query_raw, key_raw, value_rows, gate_rows, 0.0)
    branch = jnp.dot(retained, out_weight, preferred_element_type=jnp.float32)
    middle = (activations.astype(jnp.float32) + branch).astype(jnp.bfloat16)
    second = rms_norm(middle, mlp_gain)
    hidden = jnp.square(jax.nn.relu(jnp.dot(second, up_weight, preferred_element_type=jnp.float32))).astype(jnp.bfloat16)
    group_width = FF // N_TP
    hidden_parts = jnp.moveaxis(hidden.reshape(hidden.shape[0], N_TP, group_width), 1, 0)
    down_parts = down_weight.reshape(N_TP, group_width, D)

    def accumulate(running, inputs):
        part_rows, part_weight = inputs
        rounded = lax.optimization_barrier(jnp.dot(part_rows, part_weight, preferred_element_type=jnp.float32).astype(jnp.bfloat16))
        return (running + rounded.astype(jnp.float32), None)
    summed, _ = lax.scan(accumulate, jnp.zeros((hidden.shape[0], D), jnp.float32), (hidden_parts, down_parts))
    return (middle.astype(jnp.float32) + summed).astype(jnp.bfloat16)
```

```python
import functools

import jax
import jax.numpy as jnp
from jax import lax
from jax.sharding import PartitionSpec as P

HEADS = 8
HEAD_DIM = 64
BLOCK = 64
SEQ_LEN = 128


EPSILON = 1e-06


def rms_norm(rows, gain):
    floats = rows.astype(jnp.float32)
    scaled = floats * lax.rsqrt(jnp.mean(floats * floats, axis=-1, keepdims=True) + EPSILON)
    return (scaled * gain).astype(jnp.bfloat16)


def rotate(raw, cosine, sine, seqs, heads):
    half = HEAD_DIM // 2
    shaped = raw.reshape(seqs, SEQ_LEN, heads, HEAD_DIM)
    first, second = (shaped[..., :half], shaped[..., half:])
    return jnp.concatenate(
        [first * cosine - second * sine, second * cosine + first * sine], axis=-1
    )


def retain(query_raw, key_raw, value_rows, gate_rows, first_head):
    tokens = query_raw.shape[0]
    heads = query_raw.shape[1] // HEAD_DIM
    seqs = tokens // SEQ_LEN
    blocks = SEQ_LEN // BLOCK
    half = HEAD_DIM // 2
    position = jnp.arange(SEQ_LEN, dtype=jnp.float32)
    freqs = 10000.0 ** (-jnp.arange(half, dtype=jnp.float32) / half)
    angle = position[:, None] * freqs[None, :]
    cosine = jnp.cos(angle)[:, None, :]
    sine = jnp.sin(angle)[:, None, :]
    shape_five = (seqs, blocks, BLOCK, heads, HEAD_DIM)
    queries = rotate(query_raw, cosine, sine, seqs, heads).astype(jnp.bfloat16).reshape(shape_five)
    key_block = (
        (rotate(key_raw, cosine, sine, seqs, heads) * HEAD_DIM ** (-0.5))
        .astype(jnp.bfloat16)
        .reshape(shape_five)
    )
    value_block = value_rows.reshape(shape_five)
    head_index = first_head + jnp.arange(heads, dtype=jnp.float32)
    exponent = 5.0 + 4.0 * head_index / (HEADS - 1)
    log_gamma = jnp.log(1.0 - jnp.power(2.0, -exponent))
    offsets = jnp.arange(BLOCK, dtype=jnp.float32)
    distance = offsets[:, None] - offsets[None, :]
    decay_mask = jnp.where(
        distance[None] >= 0,
        jnp.exp(jnp.maximum(distance, 0.0)[None] * log_gamma[:, None, None]),
        0.0,
    )
    scores = jnp.einsum(
        "snbhd,snchd->snhbc", queries, key_block, preferred_element_type=jnp.float32
    )
    weights = (scores * decay_mask[None, None]).astype(jnp.bfloat16)
    inner = jnp.einsum(
        "snhbc,snchd->snbhd", weights, value_block, preferred_element_type=jnp.float32
    )
    query_decay = (
        queries.astype(jnp.float32)
        * jnp.exp((offsets + 1.0)[:, None] * log_gamma[None, :])[:, :, None]
    )
    key_decay = (
        key_block.astype(jnp.float32)
        * jnp.exp((BLOCK - 1.0 - offsets)[:, None] * log_gamma[None, :])[:, :, None]
    )
    block_decay = jnp.exp(BLOCK * log_gamma)[None, :, None, None]

    def advance(state, inputs):
        query_now, key_now, value_now = inputs
        carried = jnp.einsum("sbhd,shde->sbhe", query_now, state, precision=lax.Precision.HIGHEST)
        state = state * block_decay + jnp.einsum(
            "sbhd,sbhe->shde", key_now, value_now, precision=lax.Precision.HIGHEST
        )
        return (state, carried)

    initial = jnp.zeros((seqs, heads, HEAD_DIM, HEAD_DIM), jnp.float32)
    _, cross = lax.scan(
        advance,
        initial,
        (
            jnp.moveaxis(query_decay, 1, 0),
            jnp.moveaxis(key_decay, 1, 0),
            jnp.moveaxis(value_block.astype(jnp.float32), 1, 0),
        ),
    )
    mixed = (inner + jnp.moveaxis(cross, 0, 1)).reshape(tokens, heads, HEAD_DIM)
    centred = mixed - jnp.mean(mixed, axis=-1, keepdims=True)
    normed = centred * lax.rsqrt(jnp.mean(centred * centred, axis=-1, keepdims=True) + EPSILON)
    gated = normed * jax.nn.silu(gate_rows.reshape(tokens, heads, HEAD_DIM))
    return gated.reshape(tokens, heads * HEAD_DIM).astype(jnp.bfloat16)


def rotate_index(size, offset):
    return [(source, (source + offset) % size) for source in range(size)]


def partner_pairs(size):
    return [(source, source ^ 1) for source in range(size)]


def spread(block, tp):
    me = lax.axis_index("tp")
    mine = [block] + [
        lax.ppermute(block, "tp", rotate_index(tp, offset)) for offset in range(2, tp, 2)
    ]
    other = [lax.ppermute(piece, "tp", partner_pairs(tp)) for piece in mine]
    stacked = jnp.zeros((tp,) + block.shape, block.dtype)
    for step, (near, far) in enumerate(zip(mine, other)):
        owner = lax.rem(me - 2 * step + tp, tp)
        stacked = lax.dynamic_update_index_in_dim(stacked, near, owner, 0)
        stacked = lax.dynamic_update_index_in_dim(stacked, far, owner ^ 1, 0)
    return stacked


def sum_spread(parts, tp):
    me = lax.axis_index("tp")
    pairs = []
    for step in range(tp // 2):
        owner = lax.rem(me + 2 * step, tp)
        keep = lax.dynamic_index_in_dim(parts, owner, 0, keepdims=False)
        give = lax.dynamic_index_in_dim(parts, owner ^ 1, 0, keepdims=False)
        came = lax.ppermute(give, "tp", partner_pairs(tp))
        pairs.append(keep.astype(jnp.float32) + came.astype(jnp.float32))
    total = pairs[0]
    for step in range(1, tp // 2):
        total = total + lax.ppermute(
            pairs[step].astype(jnp.bfloat16), "tp", rotate_index(tp, 2 * step)
        ).astype(jnp.float32)
    return total


def share(block, rep):
    rows = block.shape[0] // rep
    part = lax.dynamic_slice_in_dim(block, lax.axis_index("rep") * rows, rows, 0)
    whole = lax.all_gather(part, ("fs", "rep"), axis=0, tiled=True)
    return whole.reshape((-1,) + block.shape)


def local(
    tp,
    rep,
    activations,
    norm_gain,
    query_weight,
    key_weight,
    value_weight,
    gate_weight,
    out_weight,
    mlp_gain,
    up_weight,
    down_weight,
):
    depth, head_width = query_weight.shape
    out_cols = out_weight.shape[1]
    small = jnp.concatenate(
        [
            jnp.concatenate([query_weight, key_weight, value_weight, gate_weight], axis=1),
            out_weight.reshape(-1, 4 * head_width),
        ],
        axis=0,
    )
    small = share(small, rep)
    fused = small[:, :depth].reshape(-1, 4 * head_width)
    out_rows = small[:, depth:].reshape(-1, head_width, out_cols)
    tokens = activations.shape[0]
    full_rows = jnp.moveaxis(spread(activations, tp), 0, 1).reshape(tokens, -1)
    normed = rms_norm(full_rows, norm_gain)
    projected = jnp.dot(normed, fused, preferred_element_type=jnp.float32)
    query_raw, key_raw, value_raw, gate_rows = jnp.split(projected, 4, axis=1)
    first_head = (lax.axis_index("tp") * (head_width // HEAD_DIM)).astype(jnp.float32)
    retained = retain(query_raw, key_raw, value_raw.astype(jnp.bfloat16), gate_rows, first_head)
    up_full = share(up_weight, rep).reshape(-1, up_weight.shape[1])
    out_full = jnp.moveaxis(out_rows, 0, 1).reshape(head_width, -1)
    out_mine = lax.all_to_all(out_full, "tp", split_axis=1, concat_axis=0, tiled=True)
    retained_full = jnp.moveaxis(spread(retained, tp), 0, 1).reshape(tokens, -1)
    branch = jnp.dot(retained_full, out_mine, preferred_element_type=jnp.float32)
    middle = (activations.astype(jnp.float32) + branch).astype(jnp.bfloat16)
    middle_rows = jnp.moveaxis(spread(middle, tp), 0, 1).reshape(tokens, -1)
    second = rms_norm(middle_rows, mlp_gain)
    up_rows = jnp.dot(second, up_full, preferred_element_type=jnp.float32)
    hidden = jnp.square(jax.nn.relu(up_rows)).astype(jnp.bfloat16)
    down_full = share(down_weight, rep)
    down_part = jnp.concatenate(
        [
            jnp.dot(hidden, down_full[f], preferred_element_type=jnp.float32)
            for f in range(down_full.shape[0])
        ],
        axis=1,
    ).astype(jnp.bfloat16)
    width = activations.shape[1]
    parts = jnp.stack([down_part[:, t * width : (t + 1) * width] for t in range(tp)])
    summed = sum_spread(parts, tp)
    return (middle.astype(jnp.float32) + summed).astype(jnp.bfloat16)


def solution(mesh):
    in_specs = (
        P(("rep", "fs"), "tp"),
        P(),
        P("fs", "tp"),
        P("fs", "tp"),
        P("fs", "tp"),
        P("fs", "tp"),
        P("tp", "fs"),
        P(),
        P("fs", "tp"),
        P("tp", "fs"),
    )
    out_specs = P(("rep", "fs"), "tp")
    body = functools.partial(local, mesh.shape["tp"], mesh.shape["rep"])
    return jax.shard_map(body, mesh=mesh, in_specs=in_specs, out_specs=out_specs, check_vma=False)
```

```python
import functools

import jax
import jax.numpy as jnp
from jax import lax
from jax.sharding import PartitionSpec as P

HEADS = 8
HEAD_DIM = 64
BLOCK = 64
SEQ_LEN = 128


EPSILON = 1e-06


def rms_norm(rows, gain):
    floats = rows.astype(jnp.float32)
    scaled = floats * lax.rsqrt(jnp.mean(floats * floats, axis=-1, keepdims=True) + EPSILON)
    return (scaled * gain).astype(jnp.bfloat16)


def rotate(raw, cosine, sine, seqs, heads):
    half = HEAD_DIM // 2
    shaped = raw.reshape(seqs, SEQ_LEN, heads, HEAD_DIM)
    first, second = (shaped[..., :half], shaped[..., half:])
    return jnp.concatenate(
        [first * cosine - second * sine, second * cosine + first * sine], axis=-1
    )


def retain(query_raw, key_raw, value_rows, gate_rows, first_head):
    tokens = query_raw.shape[0]
    heads = query_raw.shape[1] // HEAD_DIM
    seqs = tokens // SEQ_LEN
    blocks = SEQ_LEN // BLOCK
    half = HEAD_DIM // 2
    position = jnp.arange(SEQ_LEN, dtype=jnp.float32)
    freqs = 10000.0 ** (-jnp.arange(half, dtype=jnp.float32) / half)
    angle = position[:, None] * freqs[None, :]
    cosine = jnp.cos(angle)[:, None, :]
    sine = jnp.sin(angle)[:, None, :]
    shape_five = (seqs, blocks, BLOCK, heads, HEAD_DIM)
    queries = rotate(query_raw, cosine, sine, seqs, heads).astype(jnp.bfloat16).reshape(shape_five)
    key_block = (
        (rotate(key_raw, cosine, sine, seqs, heads) * HEAD_DIM ** (-0.5))
        .astype(jnp.bfloat16)
        .reshape(shape_five)
    )
    value_block = value_rows.reshape(shape_five)
    head_index = first_head + jnp.arange(heads, dtype=jnp.float32)
    exponent = 5.0 + 4.0 * head_index / (HEADS - 1)
    log_gamma = jnp.log(1.0 - jnp.power(2.0, -exponent))
    offsets = jnp.arange(BLOCK, dtype=jnp.float32)
    distance = offsets[:, None] - offsets[None, :]
    decay_mask = jnp.where(
        distance[None] >= 0,
        jnp.exp(jnp.maximum(distance, 0.0)[None] * log_gamma[:, None, None]),
        0.0,
    )
    scores = jnp.einsum(
        "snbhd,snchd->snhbc", queries, key_block, preferred_element_type=jnp.float32
    )
    weights = (scores * decay_mask[None, None]).astype(jnp.bfloat16)
    inner = jnp.einsum(
        "snhbc,snchd->snbhd", weights, value_block, preferred_element_type=jnp.float32
    )
    query_decay = (
        queries.astype(jnp.float32)
        * jnp.exp((offsets + 1.0)[:, None] * log_gamma[None, :])[:, :, None]
    )
    key_decay = (
        key_block.astype(jnp.float32)
        * jnp.exp((BLOCK - 1.0 - offsets)[:, None] * log_gamma[None, :])[:, :, None]
    )
    block_decay = jnp.exp(BLOCK * log_gamma)[None, :, None, None]

    def advance(state, inputs):
        query_now, key_now, value_now = inputs
        carried = jnp.einsum("sbhd,shde->sbhe", query_now, state, precision=lax.Precision.HIGHEST)
        state = state * block_decay + jnp.einsum(
            "sbhd,sbhe->shde", key_now, value_now, precision=lax.Precision.HIGHEST
        )
        return (state, carried)

    initial = jnp.zeros((seqs, heads, HEAD_DIM, HEAD_DIM), jnp.float32)
    _, cross = lax.scan(
        advance,
        initial,
        (
            jnp.moveaxis(query_decay, 1, 0),
            jnp.moveaxis(key_decay, 1, 0),
            jnp.moveaxis(value_block.astype(jnp.float32), 1, 0),
        ),
    )
    mixed = (inner + jnp.moveaxis(cross, 0, 1)).reshape(tokens, heads, HEAD_DIM)
    centred = mixed - jnp.mean(mixed, axis=-1, keepdims=True)
    normed = centred * lax.rsqrt(jnp.mean(centred * centred, axis=-1, keepdims=True) + EPSILON)
    gated = normed * jax.nn.silu(gate_rows.reshape(tokens, heads, HEAD_DIM))
    return gated.reshape(tokens, heads * HEAD_DIM).astype(jnp.bfloat16)


def shifted(size, offset):
    return [(source, (source + offset) % size) for source in range(size)]


def partner_pairs(size):
    return [(source, source ^ 1) for source in range(size)]


def in_order(pieces, owners):
    stacked = jnp.zeros((len(pieces),) + pieces[0].shape, pieces[0].dtype)
    for piece, owner in zip(pieces, owners):
        stacked = lax.dynamic_update_index_in_dim(stacked, piece, owner, 0)
    return stacked


def spread(block, tp):
    me = lax.axis_index("tp")
    mine = [block] + [
        lax.ppermute(block, "tp", shifted(tp, offset)) for offset in range(2, tp, 2)
    ]
    other = [lax.ppermute(piece, "tp", partner_pairs(tp)) for piece in mine]
    near = [lax.rem(me - 2 * step + tp, tp) for step in range(tp // 2)]
    stacked = in_order(mine + other, near + [owner ^ 1 for owner in near])
    return jnp.moveaxis(stacked, 0, 1).reshape(block.shape[0], -1)


def across(block, rep):
    return [block] + [lax.ppermute(block, "rep", shifted(rep, k)) for k in range(1, rep)]


def sum_spread(part, tp):
    me = lax.axis_index("tp")
    width = part.shape[1] // tp

    def columns(owner):
        return lax.dynamic_slice_in_dim(part, owner * width, width, 1)

    pairs = []
    for step in reversed(range(tp // 2)):
        owner = lax.rem(me + 2 * step, tp)
        came = lax.ppermute(columns(owner ^ 1), "tp", partner_pairs(tp))
        pair = columns(owner).astype(jnp.float32) + came.astype(jnp.float32)
        if step:
            pair = lax.ppermute(
                pair.astype(jnp.bfloat16), "tp", shifted(tp, 2 * step)
            ).astype(jnp.float32)
        pairs.append(pair)
    return sum(pairs[1:], pairs[0])


def local(
    tp,
    rep,
    activations,
    norm_gain,
    query_weight,
    key_weight,
    value_weight,
    gate_weight,
    out_weight,
    mlp_gain,
    up_weight,
    down_weight,
):
    depth, head_width = query_weight.shape
    out_cols = out_weight.shape[1]
    tokens = activations.shape[0]
    mine = lax.axis_index("rep")
    split = rep if head_width % (rep * HEAD_DIM) == 0 else 1
    part_width = head_width // split
    start = mine * part_width if split > 1 else 0

    def own(weight, axis):
        return lax.dynamic_slice_in_dim(weight, start, part_width, axis) if split > 1 else weight

    small = jnp.concatenate(
        [
            jnp.concatenate(
                [own(w, 1) for w in (query_weight, key_weight, value_weight, gate_weight)], axis=1
            ),
            own(out_weight, 0).reshape(-1, 4 * part_width),
        ],
        axis=0,
    )
    rows = small.shape[0]
    small = lax.all_gather(small, "fs", axis=0, tiled=True).reshape(-1, rows, 4 * part_width)
    fused = small[:, :depth].reshape(-1, 4 * part_width)
    out_rows = small[:, depth:].reshape(-1, part_width, out_cols)
    groups = across(activations, split)
    full_rows = jnp.concatenate([spread(block, tp) for block in groups], axis=0)
    normed = rms_norm(full_rows, norm_gain)
    projected = jnp.dot(normed, fused, preferred_element_type=jnp.float32)
    query_raw, key_raw, value_raw, gate_rows = jnp.split(projected, 4, axis=1)
    first_column = lax.axis_index("tp") * head_width + start
    first_head = (first_column // HEAD_DIM).astype(jnp.float32)
    retained = retain(query_raw, key_raw, value_raw.astype(jnp.bfloat16), gate_rows, first_head)
    out_full = jnp.moveaxis(out_rows, 0, 1).reshape(part_width, -1)
    out_mine = lax.all_to_all(out_full, "tp", split_axis=1, concat_axis=0, tiled=True)
    if split > 1:
        owners = [lax.rem(mine - k + rep, rep) for k in range(rep)]
        out_mine = in_order(across(out_mine, rep), owners)
        width = out_mine.shape[2]
        out_mine = jnp.moveaxis(out_mine.reshape(rep, tp, part_width, width), 0, 1)
        out_mine = out_mine.reshape(-1, width)
        heads = [retained[:tokens]] + [
            lax.ppermute(retained[k * tokens : (k + 1) * tokens], "rep", shifted(rep, -k))
            for k in range(1, rep)
        ]
        back = [lax.rem(mine + k, rep) for k in range(rep)]
        retained = jnp.moveaxis(in_order(heads, back), 0, 1).reshape(tokens, head_width)
    branch = jnp.dot(spread(retained, tp), out_mine, preferred_element_type=jnp.float32)
    middle = (activations.astype(jnp.float32) + branch).astype(jnp.bfloat16)

    hidden_width = up_weight.shape[1] // rep
    up_part = lax.dynamic_slice_in_dim(up_weight, mine * hidden_width, hidden_width, 1)
    up_full = lax.all_gather(up_part, "fs", axis=0, tiled=True)
    down_part = lax.dynamic_slice_in_dim(down_weight, mine * hidden_width, hidden_width, 0)
    down_full = lax.all_gather(down_part, "fs", axis=0, tiled=True)
    down_full = down_full.reshape(-1, hidden_width, down_part.shape[1])
    second = [rms_norm(spread(block, tp), mlp_gain) for block in across(middle, rep)]
    up_rows = jnp.dot(
        jnp.concatenate(second, axis=0), up_full, preferred_element_type=jnp.float32
    )
    hidden = jnp.square(jax.nn.relu(up_rows)).astype(jnp.bfloat16)
    total = middle.astype(jnp.float32)
    for k in reversed(range(rep)):
        block = hidden[k * tokens : (k + 1) * tokens]
        product = jnp.concatenate(
            [
                jnp.dot(block, down_full[f], preferred_element_type=jnp.float32).astype(jnp.bfloat16)
                for f in range(down_full.shape[0])
            ],
            axis=1,
        )
        summed = sum_spread(product, tp)
        if k:
            summed = lax.ppermute(
                summed.astype(jnp.bfloat16), "rep", shifted(rep, -k)
            ).astype(jnp.float32)
        total = total + summed
    return total.astype(jnp.bfloat16)


def solution(mesh):
    in_specs = (
        P(("rep", "fs"), "tp"),
        P(),
        P("fs", "tp"),
        P("fs", "tp"),
        P("fs", "tp"),
        P("fs", "tp"),
        P("tp", "fs"),
        P(),
        P("fs", "tp"),
        P("tp", "fs"),
    )
    out_specs = P(("rep", "fs"), "tp")
    body = functools.partial(local, mesh.shape["tp"], mesh.shape["rep"])
    return jax.shard_map(body, mesh=mesh, in_specs=in_specs, out_specs=out_specs, check_vma=False)
```

```python
import functools

import jax
import jax.numpy as jnp
from jax import lax
from jax.sharding import PartitionSpec as P

HEADS = 8
HEAD_DIM = 64
BLOCK = 64
SEQ_LEN = 128


EPSILON = 1e-06


def rms_norm(rows, gain):
    floats = rows.astype(jnp.float32)
    scaled = floats * lax.rsqrt(jnp.mean(floats * floats, axis=-1, keepdims=True) + EPSILON)
    return (scaled * gain).astype(jnp.bfloat16)


def rotate(raw, cosine, sine, seqs, heads):
    half = HEAD_DIM // 2
    shaped = raw.reshape(seqs, SEQ_LEN, heads, HEAD_DIM)
    first, second = (shaped[..., :half], shaped[..., half:])
    return jnp.concatenate(
        [first * cosine - second * sine, second * cosine + first * sine], axis=-1
    )


def retain(query_raw, key_raw, value_rows, gate_rows, first_head):
    tokens = query_raw.shape[0]
    heads = query_raw.shape[1] // HEAD_DIM
    seqs = tokens // SEQ_LEN
    blocks = SEQ_LEN // BLOCK
    half = HEAD_DIM // 2
    position = jnp.arange(SEQ_LEN, dtype=jnp.float32)
    freqs = 10000.0 ** (-jnp.arange(half, dtype=jnp.float32) / half)
    angle = position[:, None] * freqs[None, :]
    cosine = jnp.cos(angle)[:, None, :]
    sine = jnp.sin(angle)[:, None, :]
    shape_five = (seqs, blocks, BLOCK, heads, HEAD_DIM)
    queries = rotate(query_raw, cosine, sine, seqs, heads).astype(jnp.bfloat16).reshape(shape_five)
    key_block = (
        (rotate(key_raw, cosine, sine, seqs, heads) * HEAD_DIM ** (-0.5))
        .astype(jnp.bfloat16)
        .reshape(shape_five)
    )
    value_block = value_rows.reshape(shape_five)
    head_index = first_head + jnp.arange(heads, dtype=jnp.float32)
    exponent = 5.0 + 4.0 * head_index / (HEADS - 1)
    log_gamma = jnp.log(1.0 - jnp.power(2.0, -exponent))
    offsets = jnp.arange(BLOCK, dtype=jnp.float32)
    distance = offsets[:, None] - offsets[None, :]
    decay_mask = jnp.where(
        distance[None] >= 0,
        jnp.exp(jnp.maximum(distance, 0.0)[None] * log_gamma[:, None, None]),
        0.0,
    )
    scores = jnp.einsum(
        "snbhd,snchd->snhbc", queries, key_block, preferred_element_type=jnp.float32
    )
    weights = (scores * decay_mask[None, None]).astype(jnp.bfloat16)
    inner = jnp.einsum(
        "snhbc,snchd->snbhd", weights, value_block, preferred_element_type=jnp.float32
    )
    query_decay = (
        queries.astype(jnp.float32)
        * jnp.exp((offsets + 1.0)[:, None] * log_gamma[None, :])[:, :, None]
    )
    key_decay = (
        key_block.astype(jnp.float32)
        * jnp.exp((BLOCK - 1.0 - offsets)[:, None] * log_gamma[None, :])[:, :, None]
    )
    block_decay = jnp.exp(BLOCK * log_gamma)[None, :, None, None]

    def advance(state, inputs):
        query_now, key_now, value_now = inputs
        carried = jnp.einsum("sbhd,shde->sbhe", query_now, state, precision=lax.Precision.HIGHEST)
        state = state * block_decay + jnp.einsum(
            "sbhd,sbhe->shde", key_now, value_now, precision=lax.Precision.HIGHEST
        )
        return (state, carried)

    initial = jnp.zeros((seqs, heads, HEAD_DIM, HEAD_DIM), jnp.float32)
    _, cross = lax.scan(
        advance,
        initial,
        (
            jnp.moveaxis(query_decay, 1, 0),
            jnp.moveaxis(key_decay, 1, 0),
            jnp.moveaxis(value_block.astype(jnp.float32), 1, 0),
        ),
    )
    mixed = (inner + jnp.moveaxis(cross, 0, 1)).reshape(tokens, heads, HEAD_DIM)
    centred = mixed - jnp.mean(mixed, axis=-1, keepdims=True)
    normed = centred * lax.rsqrt(jnp.mean(centred * centred, axis=-1, keepdims=True) + EPSILON)
    gated = normed * jax.nn.silu(gate_rows.reshape(tokens, heads, HEAD_DIM))
    return gated.reshape(tokens, heads * HEAD_DIM).astype(jnp.bfloat16)


def shifted(size, offset):
    return [(source, (source + offset) % size) for source in range(size)]


def partner_pairs(size):
    return [(source, source ^ 1) for source in range(size)]


def in_order(pieces, owners):
    stacked = jnp.zeros((len(pieces),) + pieces[0].shape, pieces[0].dtype)
    for piece, owner in zip(pieces, owners):
        stacked = lax.dynamic_update_index_in_dim(stacked, piece, owner, 0)
    return stacked


def spread(block, tp):
    me = lax.axis_index("tp")
    mine = [block] + [
        lax.ppermute(block, "tp", shifted(tp, offset)) for offset in range(2, tp, 2)
    ]
    other = [lax.ppermute(piece, "tp", partner_pairs(tp)) for piece in mine]
    near = [lax.rem(me - 2 * step + tp, tp) for step in range(tp // 2)]
    stacked = in_order(mine + other, near + [owner ^ 1 for owner in near])
    return jnp.moveaxis(stacked, 0, 1).reshape(block.shape[0], -1)


def across(block, rep):
    return [block] + [lax.ppermute(block, "rep", shifted(rep, k)) for k in range(1, rep)]


def core_sums(part, tp):
    me = lax.axis_index("tp")
    width = part.shape[1] // tp

    def columns(owner):
        return lax.dynamic_slice_in_dim(part, owner * width, width, 1)

    sums = []
    for step in range(tp // 2):
        owner = lax.rem(me + 2 * step, tp)
        came = lax.ppermute(columns(owner ^ 1), "tp", partner_pairs(tp))
        sums.append(columns(owner).astype(jnp.float32) + came.astype(jnp.float32))
    return sums


def fold(sums, axis, pairs_of):
    total = sums[0]
    for step in range(1, len(sums)):
        total = total + lax.ppermute(
            sums[step].astype(jnp.bfloat16), axis, pairs_of(step)
        ).astype(jnp.float32)
    return total


def local(
    tp,
    rep,
    activations,
    norm_gain,
    query_weight,
    key_weight,
    value_weight,
    gate_weight,
    out_weight,
    mlp_gain,
    up_weight,
    down_weight,
):
    depth, head_width = query_weight.shape
    out_cols = out_weight.shape[1]
    tokens = activations.shape[0]
    mine = lax.axis_index("rep")
    split = rep if head_width % (rep * HEAD_DIM) == 0 else 1
    part_width = head_width // split
    start = mine * part_width if split > 1 else 0

    def own(weight, axis):
        kept = lax.slice_in_dim(weight, 0, part_width, axis=axis)
        for k in range(1, split):
            piece = lax.slice_in_dim(weight, k * part_width, (k + 1) * part_width, axis=axis)
            kept = jnp.where(mine == k, piece, kept)
        return kept

    small = jnp.concatenate(
        [
            jnp.concatenate(
                [own(w, 1) for w in (query_weight, key_weight, value_weight, gate_weight)], axis=1
            ),
            own(out_weight, 0).reshape(-1, 4 * part_width),
        ],
        axis=0,
    )
    rows = small.shape[0]
    small = lax.all_gather(small, "fs", axis=0, tiled=True).reshape(-1, rows, 4 * part_width)
    fused = small[:, :depth].reshape(-1, 4 * part_width)
    out_rows = small[:, depth:].reshape(-1, part_width, out_cols)
    groups = across(activations, split)
    full_rows = jnp.concatenate([spread(block, tp) for block in groups], axis=0)
    normed = rms_norm(full_rows, norm_gain)
    projected = jnp.dot(normed, fused, preferred_element_type=jnp.float32)
    query_raw, key_raw, value_raw, gate_rows = jnp.split(projected, 4, axis=1)
    first_column = lax.axis_index("tp") * head_width + start
    first_head = (first_column // HEAD_DIM).astype(jnp.float32)
    retained = retain(query_raw, key_raw, value_raw.astype(jnp.bfloat16), gate_rows, first_head)
    out_full = jnp.moveaxis(out_rows, 0, 1).reshape(part_width, -1)
    out_mine = lax.all_to_all(out_full, "tp", split_axis=1, concat_axis=0, tiled=True)
    if split > 1:
        owners = [lax.rem(mine - k + rep, rep) for k in range(rep)]
        out_mine = in_order(across(out_mine, rep), owners)
        width = out_mine.shape[2]
        out_mine = jnp.moveaxis(out_mine.reshape(rep, tp, part_width, width), 0, 1)
        out_mine = out_mine.reshape(-1, width)
        heads = [retained[:tokens]] + [
            lax.ppermute(retained[k * tokens : (k + 1) * tokens], "rep", shifted(rep, -k))
            for k in range(1, rep)
        ]
        back = [lax.rem(mine + k, rep) for k in range(rep)]
        retained = jnp.moveaxis(in_order(heads, back), 0, 1).reshape(tokens, head_width)
    branch = jnp.dot(spread(retained, tp), out_mine, preferred_element_type=jnp.float32)
    middle = (activations.astype(jnp.float32) + branch).astype(jnp.bfloat16)

    hidden_width = up_weight.shape[1] // rep
    up_part = lax.dynamic_slice_in_dim(up_weight, mine * hidden_width, hidden_width, 1)
    up_full = lax.all_gather(up_part, "fs", axis=0, tiled=True)
    down_part = lax.dynamic_slice_in_dim(down_weight, mine * hidden_width, hidden_width, 0)
    down_full = lax.all_gather(down_part, "fs", axis=0, tiled=True)
    down_full = down_full.reshape(-1, hidden_width, down_part.shape[1])
    second = [rms_norm(spread(block, tp), mlp_gain) for block in across(middle, rep)]
    up_rows = jnp.dot(
        jnp.concatenate(second, axis=0), up_full, preferred_element_type=jnp.float32
    )
    hidden = jnp.square(jax.nn.relu(up_rows)).astype(jnp.bfloat16)
    sums = []
    for k in range(rep):
        block = hidden[k * tokens : (k + 1) * tokens]
        product = jnp.concatenate(
            [
                jnp.dot(block, down_full[f], preferred_element_type=jnp.float32).astype(jnp.bfloat16)
                for f in range(down_full.shape[0])
            ],
            axis=1,
        )
        sums.append(core_sums(product, tp))

    def over_tp(step):
        return shifted(tp, 2 * step)

    def over_rep(step):
        return shifted(rep, -step)

    middle_row = tokens // 2
    upper = [fold([item[:middle_row] for item in group], "tp", over_tp) for group in sums]
    upper = fold(upper, "rep", over_rep)
    lower = [
        fold([group[step][middle_row:] for group in sums], "rep", over_rep)
        for step in range(tp // 2)
    ]
    lower = fold(lower, "tp", over_tp)
    summed = jnp.concatenate([upper, lower], axis=0)
    return (middle.astype(jnp.float32) + summed).astype(jnp.bfloat16)


def solution(mesh):
    in_specs = (
        P(("rep", "fs"), "tp"),
        P(),
        P("fs", "tp"),
        P("fs", "tp"),
        P("fs", "tp"),
        P("fs", "tp"),
        P("tp", "fs"),
        P(),
        P("fs", "tp"),
        P("tp", "fs"),
    )
    out_specs = P(("rep", "fs"), "tp")
    body = functools.partial(local, mesh.shape["tp"], mesh.shape["rep"])
    return jax.shard_map(body, mesh=mesh, in_specs=in_specs, out_specs=out_specs, check_vma=False)
```
